32 devices in a mesh: grp: 2 (over x), ep: 16 (over z, y, core).
Axes of the slice: x: 2, y: 2, z: 4, core: 2. Of those that a mesh axis runs over, the one named last changes fastest.
Arguments:
- tokens: bfloat16 [512, 2048], P(('grp', 'ep')), parts along dimension 0, may hold values from -6 to 6
- attn_gain: float32 [2048], replicated, may hold values from 0.1 to 1.9
- w_query: bfloat16 [2048, 1024], replicated, may hold values from -0.125 to 0.125
- w_key: bfloat16 [2048, 128], replicated, may hold values from -0.125 to 0.125
- w_value: bfloat16 [2048, 128], replicated, may hold values from -0.125 to 0.125
- w_forget: bfloat16 [2048, 2], replicated, may hold values from -0.125 to 0.125
- forget_bias: float32 [2], replicated, may hold values from -3 to 1
- w_attn_out: bfloat16 [1024, 2048], replicated, may hold values from -0.1875 to 0.1875
- cache_keys: bfloat16 [512, 1024, 128], P(('grp', 'ep')), parts along dimension 0, may hold values from -640 to 640
- cache_values: bfloat16 [512, 1024, 128], P(('grp', 'ep')), parts along dimension 0, may hold values from -6 to 6
- cache_logsum: float32 [512, 2, 1024], P(('grp', 'ep')), parts along dimension 0, may hold values from -100 to 0, as said below
- lengths: int32 [512], P(('grp', 'ep')), parts along dimension 0, may hold values from 1 to 1024, as said below
- ffn_gain: float32 [2048], replicated, may hold values from 0.1 to 1.9
- branch_gate: float32 [2048], replicated, may hold values from -0.125 to 0.125
- dense_gate: bfloat16 [2048, 4096], P(None, 'ep'), may hold values from -0.125 to 0.125
- dense_up: bfloat16 [2048, 4096], P(None, 'ep'), may hold values from -0.125 to 0.125
- dense_down: bfloat16 [4096, 2048], P('ep'), may hold values from -0.09375 to 0.09375
- expert_gate: bfloat16 [16, 2048, 512], P('ep'), may hold values from -0.125 to 0.125
- expert_up: bfloat16 [16, 2048, 512], P('ep'), may hold values from -0.125 to 0.125
- expert_down: bfloat16 [16, 512, 2048], P('ep'), may hold values from -0.25 to 0.25
- routes: int32 [512, 4], P(('grp', 'ep')), parts along dimension 0, may hold values from 0 to 15, all different within a row; in each aligned block of 16 rows (0 to 15, 16 to 31, ...) at most 8 rows name the same one
- route_weights: float32 [512, 4], P(('grp', 'ep')), parts along dimension 0, may hold values from 0.2 to 1
Outputs:
- output_rows: bfloat16 [512, 2048], P(('grp', 'ep')), parts along dimension 0
The draws below stay inside these ranges and needn't reach their ends.
There are 2 independent parts, one for each index of `grp`. The reference program is written for one: setup_inputs(seed, part) draws one part's arguments, and reference() takes and returns one part's arrays. A program takes and returns all parts, laid end to end along the dimension named above; an argument that names none is the same for every part. Nothing has to cross between parts.
Inputs may be any that keep to these rules, and one draw needn't show every extreme that they name: `lengths`: each aligned block of 16 sequences holds one with 1024 valid positions; every length is at least 128. `routes`: a row's 4 experts differ; among the rows of one device no expert is named more than 8 times. `cache_logsum`: non-increasing along positions.
All inputs are finite; a program needn't handle non-finite values.
Results may differ from the reference program's by a relative error of at most 0.012.
The reference program's roundings to bfloat16 on the way count: a program that leaves them out, or rounds other values in their place, can miss the bound.
Values may be sent and summed in bfloat16 or wider, within the bound.
No kernel may reach another device: no remote copies, remote signals or barrier semaphores. Data moves between devices by JAX's collectives and lax.ppermute only.
A program may use at most 128 MiB of HBM per device.

```python
import math
import jax
import jax.numpy as jnp
import numpy as np
from jax import lax

D = 2048
HEADS = 16
HD = 64
KEY_VALUE_HEADS = 2
EH = 512
DENSE_FF = 4096
TOPK = 4
CACHE_POSITIONS = 1024
SEQ_DEV = 16
SEQUENCE_TOTAL = 256
EXPERTS = 16
CAP = 8
N_EP = 16


def draw_lengths(key, part):
    first_key, second_key = jax.random.split(jax.random.fold_in(key, 11))
    drawn = jax.random.randint(first_key, (SEQUENCE_TOTAL,), CACHE_POSITIONS // 8, CACHE_POSITIONS + 1)
    chosen = jax.random.randint(second_key, (SEQUENCE_TOTAL // SEQ_DEV,), 0, SEQ_DEV)
    ordinal = jnp.arange(SEQUENCE_TOTAL, dtype=jnp.int32)
    filled = ordinal % SEQ_DEV == jnp.repeat(chosen, SEQ_DEV)
    return jnp.where(filled, CACHE_POSITIONS, drawn).astype(jnp.int32)


def draw_cache_keys(key, part):
    random_subkeys = jax.random.split(jax.random.fold_in(key, 21), 1)
    row_width = KEY_VALUE_HEADS * HD
    drawn = jax.random.truncated_normal(random_subkeys[0], -6.0, 6.0, (SEQUENCE_TOTAL, CACHE_POSITIONS, row_width), jnp.float32)
    return drawn.astype(jnp.bfloat16)


def draw_cache_logsum(key, part):
    random_subkeys = jax.random.split(jax.random.fold_in(key, 31), 7)
    head_shape = (SEQUENCE_TOTAL, KEY_VALUE_HEADS, 1)
    slow_share = 0.5
    slow_flag = jax.random.uniform(random_subkeys[0], head_shape) < slow_share
    slow_rate = jnp.exp(jax.random.uniform(random_subkeys[1], head_shape, jnp.float32, math.log(0.1), math.log(0.6))) / CACHE_POSITIONS
    fast_rate = jnp.exp(jax.random.uniform(random_subkeys[2], head_shape, jnp.float32, math.log(0.01), math.log(1.0 / 30.0)))
    selected_rate = jnp.where(slow_flag, slow_rate, fast_rate)
    group_member = jnp.exp(jax.random.uniform(random_subkeys[3], (SEQUENCE_TOTAL, 1, 1), jnp.float32, math.log(0.7), math.log(1.4)))
    jaggedness = jax.random.uniform(random_subkeys[4], (SEQUENCE_TOTAL, KEY_VALUE_HEADS, CACHE_POSITIONS), jnp.float32, 0.3, 1.7)
    spike_locations = jax.random.randint(random_subkeys[5], (SEQUENCE_TOTAL, KEY_VALUE_HEADS, 2), 0, CACHE_POSITIONS)
    spike_penalty = jax.random.uniform(random_subkeys[6], (SEQUENCE_TOTAL, KEY_VALUE_HEADS, 2), jnp.float32, 0.22, 0.5)
    cache_position = lax.broadcasted_iota(jnp.int32, (SEQUENCE_TOTAL, KEY_VALUE_HEADS, 2, CACHE_POSITIONS), 3)
    spike_events = jnp.sum(jnp.where(cache_position == spike_locations[..., None], spike_penalty[..., None], 0.0), axis=2)
    step_increments = -selected_rate * group_member * jaggedness - jnp.where(slow_flag, spike_events, 0.0)
    return jnp.cumsum(step_increments, axis=2)


def steps_of(own_key, shape, shards, smallest, largest):
    gain = 1.0
    for axis_at, parts in shards:
        heights = jax.random.uniform(jax.random.fold_in(jax.random.fold_in(own_key, 6), axis_at), (parts,), jnp.float32, smallest / len(shards), largest / len(shards))
        gain = gain * jnp.repeat(jnp.exp(heights), shape[axis_at] // parts).reshape((-1,) + (1,) * (len(shape) - 1 - axis_at))
    return gain


def assign_block(rng, own, number, rows, amount, top, bound, slope):
    order = jax.random.permutation(rng, amount)
    heavy_load, ordinary = load_shares(amount, rows * top, bound, slope, True), load_shares(amount, rows * top, bound, slope, False)
    places = jnp.arange(amount)

    def named(tallies, rotation):
        used = int((tallies > 0).sum())
        fixed = max(1, used // 4)
        passed = fixed + (places - fixed + rotation * (used - fixed)) % max(1, amount - fixed)
        return jnp.zeros((amount,), jnp.int32).at[order[jnp.where(places < fixed, places, passed)]].set(jnp.asarray(tallies, jnp.int32))

    tallies = jnp.where(number % 4 == 0, named(heavy_load, number // 4), named(ordinary, number - number // 4 - 1))
    mixed = jax.random.permutation(jax.random.fold_in(own, 3), amount)
    source_of, sink = mixed[0:amount // 2 * 2:2], mixed[1:amount // 2 * 2:2]
    margin = jnp.minimum(tallies[source_of] - 1, bound - tallies[sink]) // 2
    margin = jnp.where((source_of == order[0]) | (sink == order[0]) | (tallies[sink] == 0), 0, jnp.maximum(margin, 0))
    passed = jax.random.randint(jax.random.fold_in(own, 4), (amount // 2,), 0, 1 << 20) % (margin + 1)
    tallies = tallies.at[source_of].add(-passed).at[sink].add(passed)
    labels = jnp.searchsorted(jnp.cumsum(tallies), jnp.arange(rows * top), side="right").astype(jnp.int32)
    listing = labels.reshape(top, rows).T
    listing = listing[jax.random.permutation(jax.random.fold_in(own, 1), rows)]
    rotation = jax.random.randint(jax.random.fold_in(own, 2), (rows, 1), 0, top)
    return jnp.take_along_axis(listing, (jnp.arange(top)[None, :] + rotation) % top, axis=1)


def load_shares(amount, total, most, skew, full):
    loads = [(1 << 20) // math.isqrt(rank ** skew) + 1 for rank in range(1, amount + 1)]
    largest = most if full else min(most, max(-(-total // amount), total * loads[0] // sum(loads)))
    least = 1 if total - largest >= amount - 1 else 0
    counts, rest = [largest] + [least] * (amount - 1), total - largest - least * (amount - 1)
    while rest > 0:
        candidates = [i for i in range(1, amount) if counts[i] < largest] or [i for i in range(1, amount) if counts[i] < most]
        whole, left = sum([loads[i] for i in candidates]), rest
        for i in candidates:
            more = min(most - counts[i], max(1, left * loads[i] // whole), rest)
            counts[i] = counts[i] + more
            rest = rest - more
    return np.array(counts)


def bell_draw(rng, extent, spread, bound, shards=(), kind=jnp.bfloat16):
    values = spread * jax.random.normal(rng, extent, jnp.float32)
    if shards:
        values = values * steps_of(rng, extent, shards, -0.22, 0.18)
    return jnp.clip(values, -bound, bound).astype(kind)


def setup_inputs(seed: int = 0, part: int = 0) -> dict:
    seeds = jax.random.split(jax.random.key(seed), 23)
    part_keys = jax.random.split(jax.random.fold_in(seeds[22], part), 23)
    tokens = bell_draw(part_keys[0], (SEQUENCE_TOTAL, D), 1.0, 6.0, ((0, 16),))
    attn_gain = jnp.clip(1.0 + 0.18 * jax.random.normal(seeds[1], (D,), jnp.float32), 0.1, 1.9)
    w_query = bell_draw(seeds[2], (D, HEADS * HD), D ** -0.5, 0.125)
    w_key = bell_draw(seeds[3], (D, KEY_VALUE_HEADS * HD), D ** -0.5, 0.125)
    w_value = bell_draw(seeds[4], (D, KEY_VALUE_HEADS * HD), D ** -0.5, 0.125)
    w_forget = bell_draw(seeds[5], (D, KEY_VALUE_HEADS), D ** -0.5, 0.125)
    forget_bias = jnp.clip(jax.random.uniform(seeds[6], (KEY_VALUE_HEADS,), jnp.float32, -3.0, 1.0), -3.0, 1.0)
    w_attn_out = bell_draw(seeds[7], (HEADS * HD, D), (HEADS * HD) ** -0.5, 0.1875)
    cache_keys = draw_cache_keys(jax.random.fold_in(jax.random.fold_in(seeds[22], part), 71), part)
    cache_values = bell_draw(part_keys[9], (SEQUENCE_TOTAL, CACHE_POSITIONS, KEY_VALUE_HEADS * HD), 1.0, 6.0, ((0, 16),))
    cache_logsum = draw_cache_logsum(jax.random.fold_in(jax.random.fold_in(seeds[22], part), 71), part)
    lengths = draw_lengths(jax.random.fold_in(jax.random.fold_in(seeds[22], part), 71), part)
    ffn_gain = jnp.clip(1.0 + 0.18 * jax.random.normal(seeds[12], (D,), jnp.float32), 0.1, 1.9)
    branch_gate = bell_draw(seeds[13], (D,), D ** -0.5, 0.125, (), jnp.float32)
    dense_gate = bell_draw(seeds[14], (D, DENSE_FF), D ** -0.5, 0.125, ((1, 16),))
    dense_up = bell_draw(seeds[15], (D, DENSE_FF), D ** -0.5, 0.125, ((1, 16),))
    dense_down = bell_draw(seeds[16], (DENSE_FF, D), DENSE_FF ** -0.5, 0.09375, ((0, 16),))
    expert_gate = bell_draw(seeds[17], (EXPERTS, D, EH), D ** -0.5, 0.125, ((0, 16),))
    expert_up = bell_draw(seeds[18], (EXPERTS, D, EH), D ** -0.5, 0.125, ((0, 16),))
    expert_down = bell_draw(seeds[19], (EXPERTS, EH, D), EH ** -0.5, 0.25, ((0, 16),))
    routes_keys = jax.random.split(jax.random.fold_in(part_keys[20], 1), SEQUENCE_TOTAL // SEQ_DEV)
    routes_turns = jax.random.permutation(jax.random.fold_in(part_keys[20], 3), SEQUENCE_TOTAL // SEQ_DEV)
    routes = jax.vmap(lambda own, number: assign_block(jax.random.fold_in(part_keys[20], 2), own, number, SEQ_DEV, EXPERTS, TOPK, CAP, 2))(routes_keys, routes_turns).reshape((SEQUENCE_TOTAL, TOPK))
    route_weights = jnp.clip(0.2 + 0.8 * jax.random.uniform(part_keys[21], (SEQUENCE_TOTAL, TOPK), jnp.float32) ** steps_of(part_keys[21], (SEQUENCE_TOTAL, TOPK), ((0, 16),), -0.2, 0.2), 0.2, 1.0)
    return dict(tokens=tokens, attn_gain=attn_gain, w_query=w_query, w_key=w_key, w_value=w_value, w_forget=w_forget, forget_bias=forget_bias, w_attn_out=w_attn_out, cache_keys=cache_keys, cache_values=cache_values, cache_logsum=cache_logsum, lengths=lengths, ffn_gain=ffn_gain, branch_gate=branch_gate, dense_gate=dense_gate, dense_up=dense_up, dense_down=dense_down, expert_gate=expert_gate, expert_up=expert_up, expert_down=expert_down, routes=routes, route_weights=route_weights)


EPSILON = 1e-06

def norm_rows(inputs, gain_vec):
    widened = inputs.astype(jnp.float32)
    scaled = widened * lax.rsqrt(lax.optimization_barrier(jnp.mean(widened * widened, axis=-1, keepdims=True)) + EPSILON)
    return (scaled * gain_vec).astype(jnp.bfloat16)

def swiglu(row_block, w_first, w_second):
    gate_part = jnp.dot(row_block, w_first, preferred_element_type=jnp.float32)
    up_part = jnp.dot(row_block, w_second, preferred_element_type=jnp.float32)
    return (jax.nn.silu(gate_part) * up_part).astype(jnp.bfloat16)

def expert_rows(row_block, w_gate, w_up, w_down):
    middle = swiglu(row_block, w_gate, w_up)
    return jnp.dot(middle, w_down, preferred_element_type=jnp.float32).astype(jnp.bfloat16)

def reference(tokens, attn_gain, w_query, w_key, w_value, w_forget, forget_bias, w_attn_out, cache_keys, cache_values, cache_logsum, lengths, ffn_gain, branch_gate, dense_gate, dense_up, dense_down, expert_gate, expert_up, expert_down, routes, route_weights):
    group_size = HEADS // KEY_VALUE_HEADS
    scaling = 1.0 / math.sqrt(HD)
    normed = norm_rows(tokens, attn_gain)
    queries = jnp.dot(normed, w_query, preferred_element_type=jnp.float32).astype(jnp.bfloat16)
    new_keys = jnp.dot(normed, w_key, preferred_element_type=jnp.float32).astype(jnp.bfloat16)
    new_values = jnp.dot(normed, w_value, preferred_element_type=jnp.float32).astype(jnp.bfloat16)
    log_gate = jax.nn.log_sigmoid(jnp.dot(normed, w_forget, preferred_element_type=jnp.float32) + forget_bias)
    positions = lax.broadcasted_iota(jnp.int32, (SEQUENCE_TOTAL, KEY_VALUE_HEADS, CACHE_POSITIONS), 2)
    latest = lax.optimization_barrier(jnp.sum(jnp.where(positions == lengths[:, None, None] - 1, cache_logsum, 0.0), axis=2))
    offsets = (latest + log_gate)[:, :, None] - cache_logsum
    usable = positions < lengths[:, None, None]
    query_heads = queries.reshape(SEQUENCE_TOTAL, KEY_VALUE_HEADS, group_size, HD).astype(jnp.float32)
    key_heads = cache_keys.reshape(SEQUENCE_TOTAL, CACHE_POSITIONS, KEY_VALUE_HEADS, HD).astype(jnp.float32)
    value_heads = cache_values.reshape(SEQUENCE_TOTAL, CACHE_POSITIONS, KEY_VALUE_HEADS, HD).astype(jnp.float32)
    scores = jnp.einsum('bgrd,blgd->bgrl', query_heads, key_heads) * scaling
    scores = jnp.where(usable[:, :, None, :], scores + offsets[:, :, None, :], -jnp.inf)
    self_score = jnp.einsum('bgrd,bgd->bgr', query_heads, new_keys.reshape(SEQUENCE_TOTAL, KEY_VALUE_HEADS, HD).astype(jnp.float32)) * scaling
    peak_score = jnp.maximum(lax.optimization_barrier(jnp.max(scores, axis=3)), self_score)
    cache_weight = jnp.exp(scores - peak_score[..., None])
    self_weight = jnp.exp(self_score - peak_score)
    denominator = lax.optimization_barrier(jnp.sum(cache_weight, axis=3)) + self_weight
    cache_probs = (cache_weight / denominator[..., None]).astype(jnp.bfloat16)
    self_probs = (self_weight / denominator).astype(jnp.bfloat16)
    attended = jnp.einsum('bgrl,blgd->bgrd', cache_probs.astype(jnp.float32), value_heads)
    attended = attended + self_probs.astype(jnp.float32)[..., None] * new_values.reshape(SEQUENCE_TOTAL, KEY_VALUE_HEADS, 1, HD).astype(jnp.float32)
    attended = attended.reshape(SEQUENCE_TOTAL, HEADS * HD).astype(jnp.bfloat16)
    residual = tokens.astype(jnp.float32) + jnp.dot(attended, w_attn_out, preferred_element_type=jnp.float32)
    second = norm_rows(residual, ffn_gain)
    branch_share = jax.nn.sigmoid(jnp.dot(second.astype(jnp.float32), branch_gate, precision=lax.Precision.HIGHEST))
    dense_hidden = swiglu(second, dense_gate, dense_up)
    dense = jnp.dot(dense_hidden, dense_down, preferred_element_type=jnp.float32)
    expert_ids = lax.broadcasted_iota(jnp.int32, (SEQUENCE_TOTAL, TOPK, EXPERTS), 2)
    weight_table = lax.optimization_barrier(jnp.sum(jnp.where(routes[:, :, None] == expert_ids, route_weights[:, :, None], 0.0), axis=1))
    limit = N_EP * CAP

    def one_expert(carried, index):
        own_column = lax.dynamic_index_in_dim(weight_table, index, 1, keepdims=False)
        picked = jnp.nonzero(own_column > 0.0, size=limit, fill_value=SEQUENCE_TOTAL)[0].astype(jnp.int32)
        clipped = jnp.minimum(picked, SEQUENCE_TOTAL - 1)
        answer = expert_rows(second[clipped], expert_gate[index], expert_up[index], expert_down[index])
        picked_weight = jnp.where(picked < SEQUENCE_TOTAL, own_column[clipped], 0.0)
        carried = carried.at[picked].add(picked_weight[:, None] * answer.astype(jnp.float32), mode='drop')
        return (carried, None)
    routed, _ = lax.scan(one_expert, jnp.zeros((SEQUENCE_TOTAL, D), jnp.float32), jnp.arange(EXPERTS, dtype=jnp.int32))
    return (residual + branch_share[:, None] * dense + routed).astype(jnp.bfloat16)
```

```python
import math

import jax
import jax.numpy as jnp
from jax import lax
from jax.experimental import pallas as pl
from jax.experimental.pallas import tpu as pltpu
from jax.sharding import PartitionSpec as P

EPSILON = 1e-06
META = 128
NT = (((1,), (1,)), ((), ()))


def mm(a, b):
    return jnp.dot(a, b, preferred_element_type=jnp.float32)


def norm_block(widened, gain):
    scaled = widened * lax.rsqrt(jnp.mean(widened * widened, axis=-1, keepdims=True) + EPSILON)
    return (scaled * gain).astype(jnp.bfloat16)


def attention_kernel(
    lengths_ref, bias_ref, tokens_ref, attn_gain_ref, forget_ref, ffn_gain_ref, meta_ref,
    wq_hbm, wk_hbm, wv_hbm, wo_hbm, keys_hbm, values_hbm, logsum_hbm,
    residual_ref, second_ref,
    wq, wk, wv, wo, keys, values, logsum, masked_q, attended, weight_sems, cache_sems,
):
    rows, width = tokens_ref.shape
    kv_heads, span = logsum.shape[1], logsum.shape[2]
    kv_width = wk.shape[1]
    head_size = kv_width // kv_heads
    heads = wq.shape[1] // head_size
    group = heads // kv_heads
    shift = head_size.bit_length() - 1
    scaling = 1.0 / math.sqrt(head_size)
    loads = [
        pltpu.make_async_copy(s, d, weight_sems.at[i])
        for i, (s, d) in enumerate(
            ((wq_hbm, wq), (wk_hbm, wk), (wv_hbm, wv), (logsum_hbm, logsum), (wo_hbm, wo))
        )
    ]
    key_loads = [
        pltpu.make_async_copy(keys_hbm.at[b], keys.at[b], cache_sems.at[0, b]) for b in range(rows)
    ]
    value_loads = [
        pltpu.make_async_copy(values_hbm.at[b], values.at[b], cache_sems.at[1, b])
        for b in range(rows)
    ]
    for load in loads[:4]:
        load.start()
    for b in range(rows):
        key_loads[b].start()
        value_loads[b].start()
    loads[4].start()

    tokens = tokens_ref[...].astype(jnp.float32)
    normed = norm_block(tokens, attn_gain_ref[...])
    normed_wide = normed.astype(jnp.float32)
    log_gates = []
    for g in range(kv_heads):
        logit = (
            jnp.sum(normed_wide * forget_ref[g : g + 1, :].astype(jnp.float32), axis=1, keepdims=True)
            + bias_ref[g]
        )
        log_gates.append(jnp.minimum(logit, 0.0) - jnp.log1p(jnp.exp(-jnp.abs(logit))))

    lane = lax.broadcasted_iota(jnp.int32, (heads, wq.shape[1]), 1)
    own_head = lax.broadcasted_iota(jnp.int32, (heads, wq.shape[1]), 0) == (lane >> shift)
    fold_row = lax.broadcasted_iota(jnp.int32, (wq.shape[1], kv_width), 0)
    fold_lane = lax.broadcasted_iota(jnp.int32, (wq.shape[1], kv_width), 1)
    fold_target = (fold_row & (head_size - 1)) + (
        (fold_row >> (shift + group.bit_length() - 1)) << shift
    )
    fold = (fold_lane == fold_target).astype(jnp.float32).astype(jnp.bfloat16)

    loads[0].wait()
    queries = mm(normed, wq[...]).astype(jnp.bfloat16).astype(jnp.float32) * scaling
    for b in range(rows):
        masked_q[b * heads : (b + 1) * heads, :] = jnp.where(
            own_head, queries[b : b + 1, :], 0.0
        ).astype(jnp.bfloat16)
    spread_q = mm(masked_q[...], fold)
    spread_q16 = spread_q.astype(jnp.bfloat16)
    loads[1].wait()
    new_keys = mm(normed, wk[...]).astype(jnp.bfloat16).astype(jnp.float32)
    loads[2].wait()
    new_values = mm(normed, wv[...]).astype(jnp.bfloat16).astype(jnp.float32)
    loads[3].wait()
    position = lax.broadcasted_iota(jnp.int32, (1, span), 1)

    step = math.gcd(rows, 4)
    for first in range(0, rows, step):
        members = range(first, first + step)
        for b in members:
            key_loads[b].wait()
        raw = [
            lax.dot_general(
                spread_q16[b * heads : (b + 1) * heads, :], keys[b], NT,
                preferred_element_type=jnp.float32,
            )
            for b in members
        ]
        probs = []
        for b, score in zip(members, raw):
            length = lengths_ref[b]
            parts = []
            for g in range(kv_heads):
                decay = logsum[b, g : g + 1, :]
                latest = jnp.sum(jnp.where(position == length - 1, decay, 0.0), axis=1, keepdims=True)
                total = latest + log_gates[g][b : b + 1, :]
                offset = jnp.where(position < length, total - decay, -jnp.inf)
                parts.append(score[g * group : (g + 1) * group, :] + offset)
            score = jnp.concatenate(parts, axis=0)
            own = jnp.sum(
                spread_q[b * heads : (b + 1) * heads, :] * new_keys[b : b + 1, :],
                axis=1, keepdims=True,
            )
            peak = jnp.maximum(jnp.max(score, axis=1, keepdims=True), own)
            weight = jnp.exp(score - peak)
            own_weight = jnp.exp(own - peak)
            inverse = 1.0 / (jnp.sum(weight, axis=1, keepdims=True) + own_weight)
            probs.append(
                (
                    (weight * inverse).astype(jnp.bfloat16),
                    (own_weight * inverse).astype(jnp.bfloat16).astype(jnp.float32),
                )
            )
        for b in members:
            value_loads[b].wait()
        for b, (prob, own_prob) in zip(members, probs):
            mixed = mm(prob, values[b]) + own_prob * new_values[b : b + 1, :]
            attended[b * heads : (b + 1) * heads, :] = mixed.astype(jnp.bfloat16)

    wide = lax.dot_general(attended[...], fold, NT, preferred_element_type=jnp.float32)
    wide = jnp.where(own_head[None], wide.reshape(rows, heads, -1), 0.0)
    side = jnp.sum(wide, axis=1).astype(jnp.bfloat16)
    loads[4].wait()
    residual = tokens + mm(side, wo[...])
    residual_ref[...] = residual
    second_ref[:, :width] = norm_block(residual, ffn_gain_ref[...])
    second_ref[:, width:] = meta_ref[...]


def attention(
    tokens, attn_gain, w_query, w_key, w_value, w_forget, forget_bias, w_attn_out,
    cache_keys, cache_values, cache_logsum, lengths, ffn_gain, meta,
):
    rows, width = tokens.shape
    heads = w_query.shape[1] // (w_key.shape[1] // cache_logsum.shape[1])
    smem = pl.BlockSpec(memory_space=pltpu.SMEM)
    vmem = pl.BlockSpec(memory_space=pltpu.VMEM)
    hbm = pl.BlockSpec(memory_space=pl.ANY)
    return pl.pallas_call(
        attention_kernel,
        out_shape=(
            jax.ShapeDtypeStruct((rows, width), jnp.float32),
            jax.ShapeDtypeStruct((rows, width + META), jnp.bfloat16),
        ),
        in_specs=[smem, smem] + [vmem] * 5 + [hbm] * 7,
        out_specs=(vmem, vmem),
        scratch_shapes=[
            pltpu.VMEM(a.shape, a.dtype)
            for a in (w_query, w_key, w_value, w_attn_out, cache_keys, cache_values, cache_logsum)
        ]
        + [
            pltpu.VMEM((rows * heads, w_query.shape[1]), jnp.bfloat16),
            pltpu.VMEM((rows * heads, w_key.shape[1]), jnp.bfloat16),
            pltpu.SemaphoreType.DMA((5,)),
            pltpu.SemaphoreType.DMA((2, rows)),
        ],
        compiler_params=pltpu.CompilerParams(vmem_limit_bytes=36 << 20),
        name="attention",
    )(
        lengths, forget_bias, tokens, attn_gain[None], w_forget.T, ffn_gain[None], meta,
        w_query, w_key, w_value, w_attn_out, cache_keys, cache_values, cache_logsum,
    )


def feed_forward_kernel(top, piece_count, *refs):
    own_ref, gate_ref = refs[:2]
    pieces = refs[2 : 2 + piece_count]
    sources = refs[2 + piece_count : 8 + piece_count]
    outs = refs[8 + piece_count : -8]
    buffers = refs[-8:-2]
    x_ref, sems = refs[-2:]
    dense_gate, dense_up, expert_gate, expert_up, dense_down, expert_down = buffers
    loads = [
        pltpu.make_async_copy(s, d, sems.at[i]) for i, (s, d) in enumerate(zip(sources, buffers))
    ]
    for load in loads:
        load.start()
    width = dense_gate.shape[0]
    at = 0
    meta = []
    for piece in pieces:
        block = piece[...].reshape(-1, width + META)
        x_ref[at : at + block.shape[0], :] = block[:, :width]
        meta.append(block[:, width:])
        at += block.shape[0]
    meta = jnp.concatenate(meta, axis=0).astype(jnp.float32)
    weights = (
        meta[:, top : 2 * top] + meta[:, 2 * top : 3 * top] + meta[:, 3 * top : 4 * top]
    )
    own = own_ref[0].astype(jnp.float32)
    routed_weight = jnp.sum(
        jnp.where(meta[:, :top] == own, weights, 0.0), axis=1, keepdims=True
    )
    x = x_ref[...]
    share = jax.nn.sigmoid(
        jnp.sum(x.astype(jnp.float32) * gate_ref[...], axis=1, keepdims=True)
    )
    loads[0].wait()
    loads[1].wait()
    hidden = (jax.nn.silu(mm(x, dense_gate[...])) * mm(x, dense_up[...])).astype(jnp.bfloat16)
    loads[2].wait()
    loads[3].wait()
    middle = (jax.nn.silu(mm(x, expert_gate[...])) * mm(x, expert_up[...])).astype(jnp.bfloat16)
    loads[4].wait()
    loads[5].wait()
    chunk = math.gcd(width, 512)
    for c in range(0, width, chunk):
        dense = mm(hidden, dense_down[:, c : c + chunk])
        routed = mm(middle, expert_down[:, c : c + chunk]).astype(jnp.bfloat16).astype(jnp.float32)
        total = (share * dense + routed_weight * routed).astype(jnp.bfloat16)
        at = 0
        for out in outs:
            blocks, rows = out.shape[0], out.shape[1]
            out[:, :, c : c + chunk] = total[at : at + blocks * rows, :].reshape(blocks, rows, chunk)
            at += blocks * rows


def feed_forward(own, branch_gate, pieces, top, weights, out_counts):
    rows = pieces[0].shape[1]
    width = weights[0].shape[0]
    total = sum(p.shape[0] for p in pieces) * rows
    smem = pl.BlockSpec(memory_space=pltpu.SMEM)
    vmem = pl.BlockSpec(memory_space=pltpu.VMEM)
    hbm = pl.BlockSpec(memory_space=pl.ANY)

    def kernel(*refs):
        feed_forward_kernel(top, len(pieces), *refs)

    return pl.pallas_call(
        kernel,
        out_shape=tuple(
            jax.ShapeDtypeStruct((c, rows, width), jnp.bfloat16) for c in out_counts
        ),
        in_specs=[smem, vmem] + [vmem] * len(pieces) + [hbm] * 6,
        out_specs=(vmem,) * len(out_counts),
        scratch_shapes=[pltpu.VMEM(w.shape, w.dtype) for w in weights]
        + [pltpu.VMEM((total, width), jnp.bfloat16), pltpu.SemaphoreType.DMA((6,))],
        compiler_params=pltpu.CompilerParams(vmem_limit_bytes=36 << 20),
        name="feed_forward",
    )(own, branch_gate[None], *pieces, *weights)


def swap(block, mask):
    size = lax.axis_size("ep")
    return lax.ppermute(block, "ep", [(i, i ^ mask) for i in range(size)])


def wide_sum(first, *others):
    total = first.astype(jnp.float32)
    for other in others:
        total = total + other.astype(jnp.float32)
    return total


def body(
    tokens, attn_gain, w_query, w_key, w_value, w_forget, forget_bias, w_attn_out,
    cache_keys, cache_values, cache_logsum, lengths, ffn_gain, branch_gate,
    dense_gate, dense_up, dense_down, expert_gate, expert_up, expert_down,
    routes, route_weights,
):
    size = lax.axis_size("ep")
    top = routes.shape[1]
    high = lax.reduce_precision(route_weights, 8, 7)
    middle = lax.reduce_precision(route_weights - high, 8, 7)
    low = route_weights - high - middle
    meta = jnp.concatenate([routes.astype(jnp.float32), high, middle, low], axis=1)
    meta = jnp.pad(meta, ((0, 0), (0, META - 4 * top))).astype(jnp.bfloat16)
    residual, second = attention(
        tokens, attn_gain, w_query, w_key, w_value, w_forget, forget_bias, w_attn_out,
        cache_keys, cache_values, cache_logsum, lengths, ffn_gain, meta,
    )
    far = [4 * k for k in range(1, size // 4)]
    quarter = jnp.stack([second] + [swap(second, m) for m in far])
    across = swap(quarter, 2)
    pieces = [quarter, across, swap(quarter, 1), swap(across, 1)]
    own = lax.axis_index("ep")[None].astype(jnp.int32)
    weights = (
        dense_gate, dense_up, expert_gate[0], expert_up[0], dense_down, expert_down[0],
    )
    count = size // 4
    near_a, near_b, other = feed_forward(
        own, branch_gate, pieces, top, weights, (count, count, 2 * count)
    )
    arrived = swap(other, 1)
    back = swap(wide_sum(near_b, arrived[count:]).astype(jnp.bfloat16), 2)
    quarter = wide_sum(near_a, arrived[:count], back)
    sent = quarter.astype(jnp.bfloat16)
    returned = [swap(sent[k], 4 * k) for k in range(1, count)]
    return wide_sum(residual + quarter[0], *returned).astype(jnp.bfloat16)


def solution(mesh):
    rows = P(("grp", "ep"), None)
    deep = P(("grp", "ep"), None, None)
    experts = P("ep", None, None)
    return jax.shard_map(
        body,
        mesh=mesh,
        in_specs=(
            rows, P(), P(), P(), P(), P(), P(), P(), deep, deep, deep, P(("grp", "ep")),
            P(), P(), P(None, "ep"), P(None, "ep"), P("ep", None),
            experts, experts, experts, rows, rows,
        ),
        out_specs=rows,
        check_vma=False,
    )
```

```python
import math

import jax
import jax.numpy as jnp
from jax import lax
from jax.experimental import pallas as pl
from jax.experimental.pallas import tpu as pltpu
from jax.sharding import PartitionSpec as P

EPSILON = 1e-06
META = 128
NT = (((1,), (1,)), ((), ()))


def in_hbm(array):
    return pltpu.with_memory_space_constraint(array, pltpu.HBM)


def mm(a, b):
    return jnp.dot(a, b, preferred_element_type=jnp.float32)


def norm_block(widened, gain):
    scaled = widened * lax.rsqrt(jnp.mean(widened * widened, axis=-1, keepdims=True) + EPSILON)
    return (scaled * gain).astype(jnp.bfloat16)


def attention_kernel(*refs):
    sources = refs[:15]
    residual_ref, second_ref = refs[15:17]
    scratch = refs[17:]
    (
        tokens_ref, attn_gain_ref, forget_ref, lengths_ref, bias_ref, routes_ref, shares_ref,
        ffn_gain_ref, wq, wk, wv, wo, logsum, keys, values,
        masked_q, attended, weight_sems, cache_sems,
    ) = scratch
    keys_hbm, values_hbm = sources[13:]
    rows, width = tokens_ref.shape
    kv_heads, span = logsum.shape[1], logsum.shape[2]
    kv_width = wk.shape[1]
    head_size = kv_width // kv_heads
    heads = wq.shape[1] // head_size
    group = heads // kv_heads
    shift = head_size.bit_length() - 1
    scaling = 1.0 / math.sqrt(head_size)
    loads = [
        pltpu.make_async_copy(sources[i], scratch[i], weight_sems.at[i]) for i in range(13)
    ]
    key_loads = [
        pltpu.make_async_copy(keys_hbm.at[b], keys.at[b], cache_sems.at[0, b]) for b in range(rows)
    ]
    value_loads = [
        pltpu.make_async_copy(values_hbm.at[b], values.at[b], cache_sems.at[1, b])
        for b in range(rows)
    ]
    for load in loads[:11] + loads[12:]:
        load.start()
    for b in range(rows):
        key_loads[b].start()
        value_loads[b].start()
    loads[11].start()
    for load in loads[:8]:
        load.wait()

    meta_row = lax.broadcasted_iota(jnp.int32, (rows, rows), 0)
    meta_lane = lax.broadcasted_iota(jnp.int32, (rows, rows), 1)
    meta_column = lax.broadcasted_iota(jnp.int32, (rows, META), 1)
    meta = jnp.zeros((rows, META), jnp.float32)
    top = routes_ref.shape[0]
    for k in range(top):
        share = shares_ref[k : k + 1, :]
        high = share.astype(jnp.bfloat16).astype(jnp.float32)
        middle = (share - high).astype(jnp.bfloat16).astype(jnp.float32)
        low = share - high - middle
        route = routes_ref[k : k + 1, :].astype(jnp.float32)
        for part, value in enumerate((route, high, middle, low)):
            column = jnp.sum(jnp.where(meta_row == meta_lane, value, 0.0), axis=1, keepdims=True)
            meta = jnp.where(meta_column == part * top + k, column, meta)
    second_ref[:, width:] = meta.astype(jnp.bfloat16)

    tokens = tokens_ref[...].astype(jnp.float32)
    normed = norm_block(tokens, attn_gain_ref[...])
    normed_wide = normed.astype(jnp.float32)
    log_gates = []
    for g in range(kv_heads):
        logit = (
            jnp.sum(normed_wide * forget_ref[g : g + 1, :].astype(jnp.float32), axis=1, keepdims=True)
            + bias_ref[g]
        )
        log_gates.append(jnp.minimum(logit, 0.0) - jnp.log1p(jnp.exp(-jnp.abs(logit))))

    lane = lax.broadcasted_iota(jnp.int32, (heads, wq.shape[1]), 1)
    own_head = lax.broadcasted_iota(jnp.int32, (heads, wq.shape[1]), 0) == (lane >> shift)
    fold_row = lax.broadcasted_iota(jnp.int32, (wq.shape[1], kv_width), 0)
    fold_lane = lax.broadcasted_iota(jnp.int32, (wq.shape[1], kv_width), 1)
    fold_target = (fold_row & (head_size - 1)) + (
        (fold_row >> (shift + group.bit_length() - 1)) << shift
    )
    fold = (fold_lane == fold_target).astype(jnp.float32).astype(jnp.bfloat16)

    loads[8].wait()
    queries = mm(normed, wq[...]).astype(jnp.bfloat16).astype(jnp.float32) * scaling
    for b in range(rows):
        masked_q[b * heads : (b + 1) * heads, :] = jnp.where(
            own_head, queries[b : b + 1, :], 0.0
        ).astype(jnp.bfloat16)
    spread_q = mm(masked_q[...], fold)
    spread_q16 = spread_q.astype(jnp.bfloat16)
    loads[9].wait()
    new_keys = mm(normed, wk[...]).astype(jnp.bfloat16).astype(jnp.float32)
    loads[10].wait()
    new_values = mm(normed, wv[...]).astype(jnp.bfloat16).astype(jnp.float32)
    loads[12].wait()
    position = lax.broadcasted_iota(jnp.int32, (1, span), 1)

    step = math.gcd(rows, 4)
    for first in range(0, rows, step):
        members = range(first, first + step)
        for b in members:
            key_loads[b].wait()
        raw = [
            lax.dot_general(
                spread_q16[b * heads : (b + 1) * heads, :], keys[b], NT,
                preferred_element_type=jnp.float32,
            )
            for b in members
        ]
        probs = []
        for b, score in zip(members, raw):
            length = lengths_ref[b]
            parts = []
            for g in range(kv_heads):
                decay = logsum[b, g : g + 1, :]
                latest = jnp.sum(jnp.where(position == length - 1, decay, 0.0), axis=1, keepdims=True)
                total = latest + log_gates[g][b : b + 1, :]
                offset = jnp.where(position < length, total - decay, -jnp.inf)
                parts.append(score[g * group : (g + 1) * group, :] + offset)
            score = jnp.concatenate(parts, axis=0)
            own = jnp.sum(
                spread_q[b * heads : (b + 1) * heads, :] * new_keys[b : b + 1, :],
                axis=1, keepdims=True,
            )
            peak = jnp.maximum(jnp.max(score, axis=1, keepdims=True), own)
            weight = jnp.exp(score - peak)
            own_weight = jnp.exp(own - peak)
            inverse = 1.0 / (jnp.sum(weight, axis=1, keepdims=True) + own_weight)
            probs.append(
                (
                    (weight * inverse).astype(jnp.bfloat16),
                    (own_weight * inverse).astype(jnp.bfloat16).astype(jnp.float32),
                )
            )
        for b in members:
            value_loads[b].wait()
        for b, (prob, own_prob) in zip(members, probs):
            mixed = mm(prob, values[b]) + own_prob * new_values[b : b + 1, :]
            attended[b * heads : (b + 1) * heads, :] = mixed.astype(jnp.bfloat16)

    wide = lax.dot_general(attended[...], fold, NT, preferred_element_type=jnp.float32)
    wide = jnp.where(own_head[None], wide.reshape(rows, heads, -1), 0.0)
    side = jnp.sum(wide, axis=1).astype(jnp.bfloat16)
    loads[11].wait()
    residual = tokens + mm(side, wo[...])
    residual_ref[...] = residual
    second_ref[:, :width] = norm_block(residual, ffn_gain_ref[...])


def attention(operands, heads):
    tokens, w_query, w_key = operands[0], operands[8], operands[9]
    rows, width = tokens.shape
    vmem = pl.BlockSpec(memory_space=pltpu.VMEM)
    hbm = pl.BlockSpec(memory_space=pltpu.HBM)
    smem = (3, 4)
    return pl.pallas_call(
        attention_kernel,
        out_shape=(
            jax.ShapeDtypeStruct((rows, width), jnp.float32),
            jax.ShapeDtypeStruct((rows, width + META), jnp.bfloat16),
        ),
        in_specs=[hbm] * len(operands),
        out_specs=(vmem, vmem),
        scratch_shapes=[
            (pltpu.SMEM if i in smem else pltpu.VMEM)(a.shape, a.dtype)
            for i, a in enumerate(operands)
        ]
        + [
            pltpu.VMEM((rows * heads, w_query.shape[1]), jnp.bfloat16),
            pltpu.VMEM((rows * heads, w_key.shape[1]), jnp.bfloat16),
            pltpu.SemaphoreType.DMA((13,)),
            pltpu.SemaphoreType.DMA((2, rows)),
        ],
        compiler_params=pltpu.CompilerParams(vmem_limit_bytes=30 << 20),
        name="attention",
    )(*map(in_hbm, operands))


def feed_forward_kernel(top, piece_count, *refs):
    own_ref, gate_hbm = refs[:2]
    pieces = refs[2 : 2 + piece_count]
    sources = refs[2 + piece_count : 8 + piece_count] + (gate_hbm,)
    outs = refs[8 + piece_count : -9]
    buffers = refs[-9:-2]
    dense_gate, dense_up, expert_gate, expert_up, dense_down, expert_down, gate_ref = buffers
    x_ref, sems = refs[-2:]
    loads = [
        pltpu.make_async_copy(s, d, sems.at[i]) for i, (s, d) in enumerate(zip(sources, buffers))
    ]
    for load in loads:
        load.start()
    width = dense_gate.shape[0]
    at = 0
    meta = []
    for piece in pieces:
        block = piece[...].reshape(-1, width + META)
        x_ref[at : at + block.shape[0], :] = block[:, :width]
        meta.append(block[:, width:])
        at += block.shape[0]
    meta = jnp.concatenate(meta, axis=0).astype(jnp.float32)
    weights = (
        meta[:, top : 2 * top] + meta[:, 2 * top : 3 * top] + meta[:, 3 * top : 4 * top]
    )
    own = own_ref[0].astype(jnp.float32)
    routed_weight = jnp.sum(
        jnp.where(meta[:, :top] == own, weights, 0.0), axis=1, keepdims=True
    )
    x = x_ref[...]
    loads[0].wait()
    loads[1].wait()
    hidden = (jax.nn.silu(mm(x, dense_gate[...])) * mm(x, dense_up[...])).astype(jnp.bfloat16)
    loads[2].wait()
    loads[3].wait()
    middle = (jax.nn.silu(mm(x, expert_gate[...])) * mm(x, expert_up[...])).astype(jnp.bfloat16)
    loads[6].wait()
    share = jax.nn.sigmoid(
        jnp.sum(x.astype(jnp.float32) * gate_ref[...], axis=1, keepdims=True)
    )
    loads[4].wait()
    loads[5].wait()
    chunk = math.gcd(width, 512)
    for c in range(0, width, chunk):
        dense = mm(hidden, dense_down[:, c : c + chunk])
        routed = mm(middle, expert_down[:, c : c + chunk]).astype(jnp.bfloat16).astype(jnp.float32)
        total = (share * dense + routed_weight * routed).astype(jnp.bfloat16)
        at = 0
        for out in outs:
            blocks, rows = out.shape[0], out.shape[1]
            out[:, :, c : c + chunk] = total[at : at + blocks * rows, :].reshape(blocks, rows, chunk)
            at += blocks * rows


def feed_forward(own, branch_gate, pieces, top, weights, out_counts):
    rows = pieces[0].shape[1]
    width = weights[0].shape[0]
    total = sum(p.shape[0] for p in pieces) * rows
    smem = pl.BlockSpec(memory_space=pltpu.SMEM)
    vmem = pl.BlockSpec(memory_space=pltpu.VMEM)
    hbm = pl.BlockSpec(memory_space=pltpu.HBM)

    def kernel(*refs):
        feed_forward_kernel(top, len(pieces), *refs)

    return pl.pallas_call(
        kernel,
        out_shape=tuple(
            jax.ShapeDtypeStruct((c, rows, width), jnp.bfloat16) for c in out_counts
        ),
        in_specs=[smem, hbm] + [vmem] * len(pieces) + [hbm] * len(weights),
        out_specs=(vmem,) * len(out_counts),
        scratch_shapes=[pltpu.VMEM(w.shape, w.dtype) for w in weights]
        + [
            pltpu.VMEM((1, width), branch_gate.dtype),
            pltpu.VMEM((total, width), jnp.bfloat16),
            pltpu.SemaphoreType.DMA((7,)),
        ],
        compiler_params=pltpu.CompilerParams(vmem_limit_bytes=30 << 20),
        name="feed_forward",
    )(own, in_hbm(branch_gate[None]), *pieces, *map(in_hbm, weights))


def swap(block, mask):
    size = lax.axis_size("ep")
    return lax.ppermute(block, "ep", [(i, i ^ mask) for i in range(size)])


def wide_sum(first, *others):
    total = first.astype(jnp.float32)
    for other in others:
        total = total + other.astype(jnp.float32)
    return total


def body(
    tokens, attn_gain, w_query, w_key, w_value, w_forget, forget_bias, w_attn_out,
    cache_keys, cache_values, cache_logsum, lengths, ffn_gain, branch_gate,
    dense_gate, dense_up, dense_down, expert_gate, expert_up, expert_down,
    routes, route_weights,
):
    size = lax.axis_size("ep")
    top = routes.shape[1]
    heads = w_query.shape[1] * cache_logsum.shape[1] // w_key.shape[1]
    residual, second = attention(
        (
            tokens, attn_gain[None], w_forget.T, lengths, forget_bias, routes.T,
            route_weights.T, ffn_gain[None], w_query, w_key, w_value, w_attn_out,
            cache_logsum, cache_keys, cache_values,
        ),
        heads,
    )
    weights = (dense_gate, dense_up, expert_gate[0], expert_up[0], dense_down, expert_down[0])
    far = [4 * k for k in range(1, size // 4)]
    quarter = jnp.stack([second] + [swap(second, m) for m in far])
    across = swap(quarter, 2)
    pieces = [quarter, across, swap(quarter, 1), swap(across, 1)]
    own = lax.axis_index("ep")[None].astype(jnp.int32)
    count = size // 4
    near_a, near_b, other = feed_forward(
        own, branch_gate, pieces, top, weights, (count, count, 2 * count)
    )
    arrived = swap(other, 1)
    back = swap(wide_sum(near_b, arrived[count:]).astype(jnp.bfloat16), 2)
    quarter = wide_sum(near_a, arrived[:count], back)
    sent = quarter.astype(jnp.bfloat16)
    returned = [swap(sent[k], 4 * k) for k in range(1, count)]
    return wide_sum(residual + quarter[0], *returned).astype(jnp.bfloat16)


def solution(mesh):
    rows = P(("grp", "ep"), None)
    deep = P(("grp", "ep"), None, None)
    experts = P("ep", None, None)
    return jax.shard_map(
        body,
        mesh=mesh,
        in_specs=(
            rows, P(), P(), P(), P(), P(), P(), P(), deep, deep, deep, P(("grp", "ep")),
            P(), P(), P(None, "ep"), P(None, "ep"), P("ep", None),
            experts, experts, experts, rows, rows,
        ),
        out_specs=rows,
        check_vma=False,
    )
```

```python
import math

import jax
import jax.numpy as jnp
from jax import lax
from jax.experimental import pallas as pl
from jax.experimental.pallas import tpu as pltpu
from jax.sharding import PartitionSpec as P

EPSILON = 1e-06
META = 128
NT = (((1,), (1,)), ((), ()))


def in_hbm(array):
    return pltpu.with_memory_space_constraint(array, pltpu.HBM)


def mm(a, b):
    return jnp.dot(a, b, preferred_element_type=jnp.float32)


def norm_block(widened, gain):
    scaled = widened * lax.rsqrt(jnp.mean(widened * widened, axis=-1, keepdims=True) + EPSILON)
    return (scaled * gain).astype(jnp.bfloat16)


def attention_kernel(*refs):
    sources = refs[:15]
    residual_ref, second_ref = refs[15:17]
    scratch = refs[17:]
    (
        tokens_ref, attn_gain_ref, forget_ref, lengths_ref, bias_ref, routes_ref, shares_ref,
        ffn_gain_ref, wq, wk, wv, wo, logsum, keys, values,
        masked_q, attended, weight_sems, cache_sems,
    ) = scratch
    keys_hbm, values_hbm = sources[13:]
    rows, width = tokens_ref.shape
    kv_heads, span = logsum.shape[1], logsum.shape[2]
    kv_width = wk.shape[1]
    head_size = kv_width // kv_heads
    heads = wq.shape[1] // head_size
    group = heads // kv_heads
    shift = head_size.bit_length() - 1
    scaling = 1.0 / math.sqrt(head_size)
    loads = [
        pltpu.make_async_copy(sources[i], scratch[i], weight_sems.at[i]) for i in range(13)
    ]
    key_loads = [
        pltpu.make_async_copy(keys_hbm.at[b], keys.at[b], cache_sems.at[0, b]) for b in range(rows)
    ]
    value_loads = [
        pltpu.make_async_copy(values_hbm.at[b], values.at[b], cache_sems.at[1, b])
        for b in range(rows)
    ]
    for load in loads[:11] + loads[12:]:
        load.start()
    for b in range(rows):
        key_loads[b].start()
        value_loads[b].start()
    loads[11].start()
    for load in loads[:8]:
        load.wait()

    meta_row = lax.broadcasted_iota(jnp.int32, (rows, rows), 0)
    meta_lane = lax.broadcasted_iota(jnp.int32, (rows, rows), 1)
    meta_column = lax.broadcasted_iota(jnp.int32, (rows, META), 1)
    meta = jnp.zeros((rows, META), jnp.float32)
    top = routes_ref.shape[0]
    for k in range(top):
        share = shares_ref[k : k + 1, :]
        high = share.astype(jnp.bfloat16).astype(jnp.float32)
        middle = (share - high).astype(jnp.bfloat16).astype(jnp.float32)
        low = share - high - middle
        route = routes_ref[k : k + 1, :].astype(jnp.float32)
        for part, value in enumerate((route, high, middle, low)):
            column = jnp.sum(jnp.where(meta_row == meta_lane, value, 0.0), axis=1, keepdims=True)
            meta = jnp.where(meta_column == part * top + k, column, meta)
    second_ref[:, width:] = meta.astype(jnp.bfloat16)

    tokens = tokens_ref[...].astype(jnp.float32)
    normed = norm_block(tokens, attn_gain_ref[...])
    normed_wide = normed.astype(jnp.float32)
    log_gates = []
    for g in range(kv_heads):
        logit = (
            jnp.sum(normed_wide * forget_ref[g : g + 1, :].astype(jnp.float32), axis=1, keepdims=True)
            + bias_ref[g]
        )
        log_gates.append(jnp.minimum(logit, 0.0) - jnp.log1p(jnp.exp(-jnp.abs(logit))))

    lane = lax.broadcasted_iota(jnp.int32, (heads, wq.shape[1]), 1)
    own_head = lax.broadcasted_iota(jnp.int32, (heads, wq.shape[1]), 0) == (lane >> shift)
    fold_row = lax.broadcasted_iota(jnp.int32, (wq.shape[1], kv_width), 0)
    fold_lane = lax.broadcasted_iota(jnp.int32, (wq.shape[1], kv_width), 1)
    fold_target = (fold_row & (head_size - 1)) + (
        (fold_row >> (shift + group.bit_length() - 1)) << shift
    )
    fold = (fold_lane == fold_target).astype(jnp.float32).astype(jnp.bfloat16)

    loads[8].wait()
    queries = mm(normed, wq[...]).astype(jnp.bfloat16).astype(jnp.float32) * scaling
    for b in range(rows):
        masked_q[b * heads : (b + 1) * heads, :] = jnp.where(
            own_head, queries[b : b + 1, :], 0.0
        ).astype(jnp.bfloat16)
    spread_q = mm(masked_q[...], fold)
    spread_q16 = spread_q.astype(jnp.bfloat16)
    loads[9].wait()
    new_keys = mm(normed, wk[...]).astype(jnp.bfloat16).astype(jnp.float32)
    loads[10].wait()
    new_values = mm(normed, wv[...]).astype(jnp.bfloat16).astype(jnp.float32)
    loads[12].wait()
    position = lax.broadcasted_iota(jnp.int32, (1, span), 1)

    step = math.gcd(rows, 8)
    for first in range(0, rows, step):
        members = range(first, first + step)
        for b in members:
            key_loads[b].wait()
        raw = [
            lax.dot_general(
                spread_q16[b * heads : (b + 1) * heads, :], keys[b], NT,
                preferred_element_type=jnp.float32,
            )
            for b in members
        ]
        probs = []
        for b, score in zip(members, raw):
            length = lengths_ref[b]
            parts = []
            for g in range(kv_heads):
                decay = logsum[b, g : g + 1, :]
                latest = jnp.sum(jnp.where(position == length - 1, decay, 0.0), axis=1, keepdims=True)
                total = latest + log_gates[g][b : b + 1, :]
                offset = jnp.where(position < length, total - decay, -jnp.inf)
                parts.append(score[g * group : (g + 1) * group, :] + offset)
            score = jnp.concatenate(parts, axis=0)
            own = jnp.sum(
                spread_q[b * heads : (b + 1) * heads, :] * new_keys[b : b + 1, :],
                axis=1, keepdims=True,
            )
            peak = jnp.maximum(jnp.max(score, axis=1, keepdims=True), own)
            weight = jnp.exp(score - peak)
            own_weight = jnp.exp(own - peak)
            inverse = 1.0 / (jnp.sum(weight, axis=1, keepdims=True) + own_weight)
            probs.append(
                (
                    (weight * inverse).astype(jnp.bfloat16),
                    (own_weight * inverse).astype(jnp.bfloat16).astype(jnp.float32),
                )
            )
        for b in members:
            value_loads[b].wait()
        for b, (prob, own_prob) in zip(members, probs):
            mixed = mm(prob, values[b]) + own_prob * new_values[b : b + 1, :]
            attended[b * heads : (b + 1) * heads, :] = mixed.astype(jnp.bfloat16)

    wide = lax.dot_general(attended[...], fold, NT, preferred_element_type=jnp.float32)
    wide = jnp.where(own_head[None], wide.reshape(rows, heads, -1), 0.0)
    side = jnp.sum(wide, axis=1).astype(jnp.bfloat16)
    loads[11].wait()
    residual = tokens + mm(side, wo[...])
    residual_ref[...] = residual
    second_ref[:, :width] = norm_block(residual, ffn_gain_ref[...])


def attention(operands, heads):
    tokens, w_query, w_key = operands[0], operands[8], operands[9]
    rows, width = tokens.shape
    vmem = pl.BlockSpec(memory_space=pltpu.VMEM)
    hbm = pl.BlockSpec(memory_space=pltpu.HBM)
    smem = (3, 4)
    return pl.pallas_call(
        attention_kernel,
        out_shape=(
            jax.ShapeDtypeStruct((rows, width), jnp.float32),
            jax.ShapeDtypeStruct((rows, width + META), jnp.bfloat16),
        ),
        in_specs=[hbm] * len(operands),
        out_specs=(vmem, vmem),
        scratch_shapes=[
            (pltpu.SMEM if i in smem else pltpu.VMEM)(a.shape, a.dtype)
            for i, a in enumerate(operands)
        ]
        + [
            pltpu.VMEM((rows * heads, w_query.shape[1]), jnp.bfloat16),
            pltpu.VMEM((rows * heads, w_key.shape[1]), jnp.bfloat16),
            pltpu.SemaphoreType.DMA((13,)),
            pltpu.SemaphoreType.DMA((2, rows)),
        ],
        compiler_params=pltpu.CompilerParams(vmem_limit_bytes=30 << 20),
        name="attention",
    )(*map(in_hbm, operands))


def feed_forward_kernel(top, piece_count, *refs):
    own_ref, gate_hbm = refs[:2]
    pieces = refs[2 : 2 + piece_count]
    sources = refs[2 + piece_count : 8 + piece_count] + (gate_hbm,)
    outs = refs[8 + piece_count : -9]
    buffers = refs[-9:-2]
    dense_gate, dense_up, expert_gate, expert_up, dense_down, expert_down, gate_ref = buffers
    x_ref, sems = refs[-2:]
    loads = [
        pltpu.make_async_copy(s, d, sems.at[i]) for i, (s, d) in enumerate(zip(sources, buffers))
    ]
    for load in loads:
        load.start()
    width = dense_gate.shape[0]
    at = 0
    meta = []
    for piece in pieces:
        block = piece[...].reshape(-1, width + META)
        x_ref[at : at + block.shape[0], :] = block[:, :width]
        meta.append(block[:, width:])
        at += block.shape[0]
    meta = jnp.concatenate(meta, axis=0).astype(jnp.float32)
    weights = (
        meta[:, top : 2 * top] + meta[:, 2 * top : 3 * top] + meta[:, 3 * top : 4 * top]
    )
    own = own_ref[0].astype(jnp.float32)
    routed_weight = jnp.sum(
        jnp.where(meta[:, :top] == own, weights, 0.0), axis=1, keepdims=True
    )
    x = x_ref[...]
    loads[0].wait()
    loads[1].wait()
    hidden = (jax.nn.silu(mm(x, dense_gate[...])) * mm(x, dense_up[...])).astype(jnp.bfloat16)
    loads[2].wait()
    loads[3].wait()
    middle = (jax.nn.silu(mm(x, expert_gate[...])) * mm(x, expert_up[...])).astype(jnp.bfloat16)
    loads[6].wait()
    share = jax.nn.sigmoid(
        jnp.sum(x.astype(jnp.float32) * gate_ref[...], axis=1, keepdims=True)
    )
    loads[4].wait()
    loads[5].wait()
    chunk = math.gcd(width, 512)
    for c in range(0, width, chunk):
        dense = mm(hidden, dense_down[:, c : c + chunk])
        routed = mm(middle, expert_down[:, c : c + chunk]).astype(jnp.bfloat16).astype(jnp.float32)
        total = (share * dense + routed_weight * routed).astype(jnp.bfloat16)
        at = 0
        for out in outs:
            blocks, rows = out.shape[0], out.shape[1]
            out[:, :, c : c + chunk] = total[at : at + blocks * rows, :].reshape(blocks, rows, chunk)
            at += blocks * rows


def feed_forward(own, branch_gate, pieces, top, weights, out_counts):
    rows = pieces[0].shape[1]
    width = weights[0].shape[0]
    total = sum(p.shape[0] for p in pieces) * rows
    smem = pl.BlockSpec(memory_space=pltpu.SMEM)
    vmem = pl.BlockSpec(memory_space=pltpu.VMEM)
    hbm = pl.BlockSpec(memory_space=pltpu.HBM)

    def kernel(*refs):
        feed_forward_kernel(top, len(pieces), *refs)

    return pl.pallas_call(
        kernel,
        out_shape=tuple(
            jax.ShapeDtypeStruct((c, rows, width), jnp.bfloat16) for c in out_counts
        ),
        in_specs=[smem, hbm] + [vmem] * len(pieces) + [hbm] * len(weights),
        out_specs=(vmem,) * len(out_counts),
        scratch_shapes=[pltpu.VMEM(w.shape, w.dtype) for w in weights]
        + [
            pltpu.VMEM((1, width), branch_gate.dtype),
            pltpu.VMEM((total, width), jnp.bfloat16),
            pltpu.SemaphoreType.DMA((7,)),
        ],
        compiler_params=pltpu.CompilerParams(vmem_limit_bytes=30 << 20),
        name="feed_forward",
    )(own, in_hbm(branch_gate[None]), *pieces, *map(in_hbm, weights))


def swap(block, mask):
    size = lax.axis_size("ep")
    return lax.ppermute(block, "ep", [(i, i ^ mask) for i in range(size)])


def wide_sum(first, *others):
    total = first.astype(jnp.float32)
    for other in others:
        total = total + other.astype(jnp.float32)
    return total


def body(
    tokens, attn_gain, w_query, w_key, w_value, w_forget, forget_bias, w_attn_out,
    cache_keys, cache_values, cache_logsum, lengths, ffn_gain, branch_gate,
    dense_gate, dense_up, dense_down, expert_gate, expert_up, expert_down,
    routes, route_weights,
):
    size = lax.axis_size("ep")
    top = routes.shape[1]
    heads = w_query.shape[1] * cache_logsum.shape[1] // w_key.shape[1]
    residual, second = attention(
        (
            tokens, attn_gain[None], w_forget.T, lengths, forget_bias, routes.T,
            route_weights.T, ffn_gain[None], w_query, w_key, w_value, w_attn_out,
            cache_logsum, cache_keys, cache_values,
        ),
        heads,
    )
    weights = (dense_gate, dense_up, expert_gate[0], expert_up[0], dense_down, expert_down[0])
    far = [4 * k for k in range(1, size // 4)]
    quarter = jnp.stack([second] + [swap(second, m) for m in far])
    across = swap(quarter, 2)
    pieces = [quarter, across, swap(quarter, 1), swap(across, 1)]
    own = lax.axis_index("ep")[None].astype(jnp.int32)
    count = size // 4
    half = count // 2
    spans = ((0, half), (half, count))
    sizes = (half, count - half)
    *near, other = feed_forward(
        own, branch_gate, pieces, top, weights, sizes + sizes + (2 * count,)
    )
    near_a, near_b = near[:2], near[2:]
    arrived = swap(other, 1)
    arrived_a, arrived_b = arrived[:count], arrived[count:]
    sum_b = [
        wide_sum(part, arrived_b[lo:hi]).astype(jnp.bfloat16)
        for part, (lo, hi) in zip(near_b, spans)
    ]
    far_back = swap(sum_b[1], 2)
    near_back = swap(sum_b[0], 2)
    far_sum = wide_sum(near_a[1], arrived_a[half:], far_back).astype(jnp.bfloat16)
    returned = [swap(far_sum[k - half], 4 * k) for k in range(half, count)]
    near_sum = wide_sum(near_a[0], arrived_a[:half], near_back)
    near_sent = near_sum.astype(jnp.bfloat16)
    returned += [swap(near_sent[k], 4 * k) for k in range(1, half)]
    return wide_sum(residual + near_sum[0], *returned).astype(jnp.bfloat16)


def solution(mesh):
    rows = P(("grp", "ep"), None)
    deep = P(("grp", "ep"), None, None)
    experts = P("ep", None, None)
    return jax.shard_map(
        body,
        mesh=mesh,
        in_specs=(
            rows, P(), P(), P(), P(), P(), P(), P(), deep, deep, deep, P(("grp", "ep")),
            P(), P(), P(None, "ep"), P(None, "ep"), P("ep", None),
            experts, experts, experts, rows, rows,
        ),
        out_specs=rows,
        check_vma=False,
    )
```
